256 devices in a mesh: sp: 32 (over z, y), dp: 8 (over x, core).
Axes of the slice: x: 4, y: 4, z: 8, core: 2. Of those that a mesh axis runs over, the one named last changes fastest.
Arguments:
- queries: bfloat16 [32768, 6144], P(('dp', 'sp')), may hold values from -360 to 360
- latent: bfloat16 [32768, 1024], P(('dp', 'sp')), may hold values from -6 to 6
- rope_key: bfloat16 [32768, 64], P(('dp', 'sp')), may hold values from -6 to 6
- latent_gain: float32 [1024], replicated, may hold values from 0.1 to 1.9
- kv_weight: bfloat16 [1024, 8192], P(None, 'dp'), may hold values from -0.1875 to 0.1875
- gate: bfloat16 [32768, 4096], P(('dp', 'sp')), may hold values from -6 to 6
- out_gain: float32 [4096], replicated, may hold values from 0.1 to 1.9
Outputs:
- attended: bfloat16 [32768, 4096], P(('dp', 'sp'))
The draws below stay inside these ranges and needn't reach their ends.
All inputs are finite; a program needn't handle non-finite values.
Results may differ from the reference program's by a relative error of at most 0.007.
Values may be sent and summed in bfloat16 or wider, within the bound.
A program may use at most 128 MiB of HBM per device.

```python
import jax
import jax.numpy as jnp
from jax import lax

HEADS = 32
NOPE = 128
ROPE = 64
VDIM = 128
KV_RANK = 1024
SEQ_LEN = 4096
TOKENS = 32768


def draw_queries(key, part):
    values = jax.random.normal(key, (TOKENS, HEADS * (NOPE + ROPE)), jnp.float32)
    values = jnp.clip(values, -6.0, 6.0)
    return values.astype(jnp.bfloat16)


def steps_of(stream_key, extent, shards, low, largest):
    loudness = 1.0
    for dim, blocks in shards:
        steps = jax.random.uniform(jax.random.fold_in(jax.random.fold_in(stream_key, 6), dim), (blocks,), jnp.float32, low / len(shards), largest / len(shards))
        loudness = loudness * jnp.repeat(jnp.exp(steps), extent[dim] // blocks).reshape((-1,) + (1,) * (len(extent) - 1 - dim))
    return loudness


def bell_draw(own_key, shape, spread, limit, pieces=(), held_as=jnp.bfloat16):
    loudness = steps_of(own_key, shape, pieces, -0.22, 0.18) if pieces else 1.0
    values = jax.random.normal(own_key, shape, jnp.float32) * spread * loudness
    return jnp.minimum(jnp.maximum(values, -limit), limit).astype(held_as)


def setup_inputs(seed: int = 0) -> dict:
    streams_of = jax.random.split(jax.random.key(seed), 8)
    return {
        "queries": draw_queries(jax.random.fold_in(streams_of[7], 71), 0),
        "latent": bell_draw(streams_of[1], (TOKENS, KV_RANK), 1.0, 6.0, ((0, 256),)),
        "rope_key": bell_draw(streams_of[2], (TOKENS, ROPE), 1.0, 6.0, ((0, 256),)),
        "latent_gain": jnp.clip(1.0 + 0.18 * jax.random.normal(streams_of[3], (KV_RANK,), jnp.float32), 0.1, 1.9),
        "kv_weight": bell_draw(streams_of[4], (KV_RANK, HEADS * (NOPE + VDIM)), KV_RANK ** -0.5, 0.1875, ((1, 8),)),
        "gate": bell_draw(streams_of[5], (TOKENS, HEADS * VDIM), 1.0, 6.0, ((0, 256),)),
        "out_gain": jnp.clip(1.0 + 0.18 * jax.random.normal(streams_of[6], (HEADS * VDIM,), jnp.float32), 0.1, 1.9),
    }


EPS = 1e-06
THETA = 10000.0

def rotary(values, position):
    half_width = values.shape[-1] // 2
    inverse = THETA ** (-jnp.arange(half_width, dtype=jnp.float32) / half_width)
    angles = position.astype(jnp.float32)[:, None] * inverse[None, :]
    if values.ndim == 3:
        angles = angles[:, None, :]
    cosine = jnp.cos(angles)
    sine_part = jnp.sin(angles)
    front_half = values[..., :half_width].astype(jnp.float32)
    back_half = values[..., half_width:].astype(jnp.float32)
    turned = jnp.concatenate([front_half * cosine - back_half * sine_part, back_half * cosine + front_half * sine_part], axis=-1)
    return turned.astype(jnp.bfloat16)

def attend(query_block, keys_plain, keys_rotated, values):
    scores = jnp.einsum('qhd,khd->hqk', query_block[..., :NOPE].astype(jnp.float32), keys_plain.astype(jnp.float32))
    scores = scores + jnp.einsum('qhr,kr->hqk', query_block[..., NOPE:].astype(jnp.float32), keys_rotated.astype(jnp.float32))
    scores = scores * (NOPE + ROPE) ** (-0.5)
    row_max = lax.optimization_barrier(jnp.max(scores, axis=-1, keepdims=True))
    raised = jnp.exp(scores - row_max)
    weights = (raised / lax.optimization_barrier(jnp.sum(raised, axis=-1, keepdims=True))).astype(jnp.bfloat16)
    result = jnp.einsum('hqk,khd->qhd', weights.astype(jnp.float32), values.astype(jnp.float32))
    return result.astype(jnp.bfloat16)

def reference(queries, latent, rope_key, latent_gain, kv_weight, gate, out_gain):
    rows_all = queries.shape[0]
    position = jnp.arange(rows_all, dtype=jnp.int32) % SEQ_LEN
    widened = latent.astype(jnp.float32)
    normed = (widened * lax.rsqrt(lax.optimization_barrier(jnp.mean(widened * widened, axis=-1, keepdims=True)) + EPS) * latent_gain.astype(jnp.float32)).astype(jnp.bfloat16)
    keyval = jnp.dot(normed, kv_weight, preferred_element_type=jnp.float32).astype(jnp.bfloat16)
    head_queries = queries.reshape(rows_all, HEADS, NOPE + ROPE)
    head_queries = jnp.concatenate([head_queries[..., :NOPE], rotary(head_queries[..., NOPE:], position)], axis=-1)
    keys_rotated = rotary(rope_key, position)
    seq_count = rows_all // SEQ_LEN
    block_rows = min(512, SEQ_LEN)
    block_count = SEQ_LEN // block_rows

    def one_sequence(operands):
        query_seq, kv_seq, rope_seq = operands
        keys_plain = kv_seq[..., :NOPE]
        values = kv_seq[..., NOPE:]
        blocks = query_seq.reshape(block_count, block_rows, HEADS, NOPE + ROPE)
        result = lax.map(lambda piece_rows: attend(piece_rows, keys_plain, rope_seq, values), blocks)
        return result.reshape(SEQ_LEN, HEADS * VDIM)
    heads_out = lax.map(one_sequence, (head_queries.reshape(seq_count, SEQ_LEN, HEADS, NOPE + ROPE), keyval.reshape(seq_count, SEQ_LEN, HEADS, NOPE + VDIM), keys_rotated.reshape(seq_count, SEQ_LEN, ROPE)))
    heads_out = heads_out.reshape(rows_all, HEADS * VDIM)
    gated_rows = heads_out.astype(jnp.float32) * jax.nn.silu(gate.astype(jnp.float32))
    scale_rows = lax.rsqrt(lax.optimization_barrier(jnp.mean(gated_rows * gated_rows, axis=-1, keepdims=True)) + EPS)
    return (gated_rows * scale_rows * out_gain.astype(jnp.float32)).astype(jnp.bfloat16)
```

```python
import functools

import jax
import jax.numpy as jnp
import numpy as np
from jax import lax
from jax.experimental import pallas as pl
from jax.experimental.pallas import tpu as pltpu
from jax.sharding import PartitionSpec as P

HEADS = 32
NOPE = 128
ROPE = 64
VDIM = 128
QDIM = NOPE + ROPE
PAIR = 2 * QDIM
KDIM = 256
CHUNK = 1024

EPS = 1e-06
THETA = 10000.0
LOG2E = 1.4426950408889634

MESH = pl.DeviceIdType.MESH
DN_T = (((1,), (1,)), ((), ()))

ORDER = (
    (0, 0), (1, 0), (3, 0), (0, 3), (0, 1), (2, 0), (1, 3), (1, 1),
    (3, 1), (3, 3), (0, 2), (2, 1), (2, 3), (1, 2), (3, 2), (2, 2),
)
QUERIES_AT = 11


def turn(x, cosine, sine, mask):
    partner = jnp.where(mask, pltpu.roll(x, 96, 1), pltpu.roll(x, 32, 1))
    return x * cosine + partner * sine


def kernel(
    q_ref, lat_ref, rk_ref, lgain_ref, w_ref, gate_ref, ogain_ref, ta_ref, tb_ref, ka_ref, kb_ref,
    out_ref,
    w_v, q_v, gate_v, silu_v, own_lat, own_rk, latb, rkb, qb, kbuf, vbuf, ob, orecv,
    w_sem, q_sem, gate_sem, own_send, lat_send, lat_recv, rk_send, rk_recv,
    q_send, q_recv, o_send, o_recv,
):
    s, d = lax.axis_index("sp"), lax.axis_index("dp")
    rows = lat_ref.shape[0]
    z, y = s // 4, s % 4
    x, c = d // 2, d % 2
    k, par = z // 2, z % 2
    m = par * 4 + y
    seq = 2 * ((y + 4 - par) % 4) + par
    home = c * 4 + (x + c) % 4
    pairs = 2

    def send(src, dst, ssem, rsem, ts, td):
        same = (ts == s) & (td == d)

        @pl.when(jnp.logical_not(same))
        def _():
            pltpu.make_async_remote_copy(
                src, dst, ssem, rsem, device_id={"sp": ts, "dp": td}, device_id_type=MESH
            ).start()

        @pl.when(same)
        def _():
            pltpu.make_async_copy(src, dst, rsem).start()

    def sent(src, dst, ssem, rsem, ts, td):
        same = (ts == s) & (td == d)

        @pl.when(jnp.logical_not(same))
        def _():
            pltpu.make_async_remote_copy(
                src, dst, ssem, rsem, device_id={"sp": ts, "dp": td}, device_id_type=MESH
            ).wait_send()

    def arrived(dst, rsem):
        pltpu.make_async_copy(dst, dst, rsem).wait()

    w_copy = pltpu.make_async_copy(w_ref, w_v, w_sem)
    q_copy = pltpu.make_async_copy(q_ref, q_v, q_sem)
    gate_copy = pltpu.make_async_copy(gate_ref, gate_v, gate_sem)
    q_copy.start()
    w_copy.start()
    gate_copy.start()

    wide = lat_ref[...].astype(jnp.float32)
    scale = lax.rsqrt(jnp.mean(wide * wide, axis=-1, keepdims=True) + EPS)
    own_lat[...] = (wide * scale * lgain_ref[...]).astype(jnp.bfloat16)
    half = ROPE // 2
    kca, ksa, kcb, ksb = ka_ref[0], ka_ref[1], kb_ref[0, s], kb_ref[1, s]
    kc, ks = kca * kcb - ksa * ksb, ksa * kcb + kca * ksb
    raw = rk_ref[...].astype(jnp.float32)
    u1, u2 = raw[:half], raw[half:]
    own_rk[:half] = (u1 * kc - u2 * ks).astype(jnp.bfloat16)
    own_rk[half:] = (u2 * kc + u1 * ks).astype(jnp.bfloat16)

    ones = jnp.ones((rows, 128), jnp.bfloat16)

    def ones_step(i, carry):
        at = pl.ds(pl.multiple_of(i * rows, rows), rows)
        for h in range(4):
            vbuf[h, at, VDIM:] = ones
        return carry

    lax.fori_loop(0, vbuf.shape[1] // rows, ones_step, 0)

    first_block = k * 4 + y
    first_to = ((2 * k + c) * 4 + (x + c) % 4, 2 * y + par)
    own_sends = [
        (own_lat, latb.at[first_block, par], own_send.at[0], lat_recv.at[first_block, par], *first_to),
        (own_rk, rkb.at[first_block, par], own_send.at[1], rk_recv.at[first_block, par], *first_to),
    ]
    for args in own_sends:
        send(*args)

    lane = lax.broadcasted_iota(jnp.int32, (rows, 128), 1)
    mask = (lane % 64) < 32
    sign = jnp.where(mask, -1.0, 1.0).astype(jnp.float32)
    ca, sa, cb, sb = ta_ref[0], ta_ref[1], tb_ref[0, s], tb_ref[1, s]
    cosine, sine = ca * cb - sa * sb, (sa * cb + ca * sb) * sign
    cosine_high, sine_high = pltpu.roll(cosine, 64, 1), pltpu.roll(sine, 64, 1)
    q_copy.wait()
    for i in range(HEADS // 2):
        at = slice(i * PAIR + 128, i * PAIR + 256)
        q_v[:, at] = turn(q_v[:, at].astype(jnp.float32), cosine, sine, mask).astype(jnp.bfloat16)
        at = slice(i * PAIR + 256, i * PAIR + 384)
        q_v[:, at] = turn(
            q_v[:, at].astype(jnp.float32), cosine_high, sine_high, mask
        ).astype(jnp.bfloat16)
    query_sends = [
        (
            q_v.at[:, pl.ds((t * pairs + p) * PAIR, PAIR)], qb.at[m, p],
            q_send.at[t, p], q_recv.at[m, p], k * 8 + home, jnp.int32(t),
        )
        for p in range(pairs)
        for t in range(8)
    ]
    gate_copy.wait()
    for i in range(16):
        at = slice(i * 256, (i + 1) * 256)
        g = gate_v[:, at].astype(jnp.float32)
        silu_v[i] = g / (1.0 + jnp.exp(-g))
    w_copy.wait()

    low = lax.broadcasted_iota(jnp.int32, (2 * rows, 128), 1) < 64

    def place(i):
        dk, dx = jnp.int32(0), jnp.int32(0)
        for n, (a, b) in enumerate(ORDER):
            dk = jnp.where(i == n, a, dk)
            dx = jnp.where(i == n, b, dx)
        return dk, dx, ((k + dk) % 4) * 4 + (x + dx) % 4

    def forwards(i, act):
        dk, dx, block = place(i)
        own = dx == 0
        ways = (
            (own | ((dx == 3) & (dk < 2)), s, 2 * ((x + 1) % 4) + c),
            (own | ((dx == 1) & (dk >= 2)), s, 2 * ((x + 3) % 4) + c),
            (own & ((dk == 0) | ((dk == 3) & (c == 0))), ((z + 2) % 8) * 4 + y, d),
            (own & ((dk == 0) | ((dk == 1) & (c == 1))), ((z + 6) % 8) * 4 + y, d),
            (None, s, 2 * x + 1 - c),
        )
        for n, (when, ts, td) in enumerate(ways):
            def go(n=n, ts=ts, td=td):
                for buf, ssem, rsem in ((latb, lat_send, lat_recv), (rkb, rk_send, rk_recv)):
                    act(pltpu.make_async_remote_copy(
                        buf.at[block, c], buf.at[block, c], ssem.at[i, n], rsem.at[block, c],
                        device_id={"sp": ts, "dp": td}, device_id_type=MESH,
                    ))

            if when is None:
                go()
            else:
                pl.when(when)(go)

    def key_step(i, carry):
        _, _, block = place(i)
        arrived(latb.at[block, c], lat_recv.at[block, c])
        arrived(rkb.at[block, c], rk_recv.at[block, c])
        forwards(i, lambda copy: copy.start())

        @pl.when(i == QUERIES_AT)
        def _():
            for args in query_sends:
                send(*args)

        arrived(latb.at[block, 1 - c], lat_recv.at[block, 1 - c])
        arrived(rkb.at[block, 1 - c], rk_recv.at[block, 1 - c])
        at = pl.ds(pl.multiple_of(i * 2 * rows, 2 * rows), 2 * rows)
        normed = latb[block].reshape(2 * rows, lat_ref.shape[1])
        both_rk = jnp.concatenate([rkb[block, 0], rkb[block, 1]], axis=1).astype(jnp.float32)
        rot = jnp.concatenate([both_rk, jnp.zeros_like(both_rk)], axis=0).T
        rot_high = pltpu.roll(rot, 64, 1)
        for h in range(4):
            both = jnp.dot(
                normed, w_v[:, h * 256 : (h + 1) * 256], preferred_element_type=jnp.float32
            )
            plain = both[:, :NOPE]
            if h % 2 == 0:
                first, second = plain, rot
            else:
                moved = pltpu.roll(plain, 64, 1)
                first = jnp.where(low, 0.0, moved)
                second = jnp.where(low, moved, rot_high)
            kbuf[h, at, :128] = first.astype(jnp.bfloat16)
            kbuf[h, at, 128:] = second.astype(jnp.bfloat16)
            vbuf[h, at, :VDIM] = both[:, NOPE:].astype(jnp.bfloat16)
        return carry

    lax.fori_loop(0, 16, key_step, 0)

    factor = LOG2E * QDIM ** -0.5
    n_chunks = kbuf.shape[1] // CHUNK

    def output_send(j, p):
        return (ob.at[j, p], orecv.at[d, p], o_send.at[j, p], o_recv.at[d, p], k * 8 + j, seq)

    def query_step(i, carry):
        r, p = (i // pairs + m // 2) % 4, i % pairs
        for part in range(2):
            arrived(qb.at[2 * r + part, p], q_recv.at[2 * r + part, p])
        for odd in range(2):
            h = 2 * p + odd
            at = slice(odd * 128, odd * 128 + KDIM)
            q = jnp.concatenate([qb[2 * r, p, :, at], qb[2 * r + 1, p, :, at]], axis=0)

            def score(j):
                return lax.dot_general(
                    q, kbuf[h, j * CHUNK : (j + 1) * CHUNK], DN_T, preferred_element_type=jnp.float32
                )

            following = score(0)
            for j in range(n_chunks):
                scores = following
                if j + 1 < n_chunks:
                    following = score(j + 1)
                top = jnp.max(scores, axis=-1, keepdims=True)
                if j:
                    top = jnp.maximum(top, before)
                raised = jnp.exp2((scores - top) * factor).astype(jnp.bfloat16)
                part_total = jnp.dot(
                    raised, vbuf[h, j * CHUNK : (j + 1) * CHUNK], preferred_element_type=jnp.float32
                )
                total = total * jnp.exp2((before - top) * factor) + part_total if j else part_total
                before = top
            result = (total[:, :VDIM] / total[:, VDIM:]).astype(jnp.bfloat16)
            at = slice(odd * VDIM, (odd + 1) * VDIM)
            ob[2 * r, p, :, at] = result[:rows]
            ob[2 * r + 1, p, :, at] = result[rows:]
        send(*output_send(2 * r, p))
        send(*output_send(2 * r + 1, p))
        return carry

    lax.fori_loop(0, 4 * pairs, query_step, 0)

    square = jnp.zeros((rows, 1), jnp.float32)
    for p in range(pairs):
        for t in range(8):
            arrived(orecv.at[t, p], o_recv.at[t, p])
            gated = orecv[t, p].astype(jnp.float32) * silu_v[t * pairs + p]
            silu_v[t * pairs + p] = gated
            square = square + jnp.sum(gated * gated, axis=-1, keepdims=True)
    scale = lax.rsqrt(square / (HEADS * VDIM) + EPS)
    for i in range(16):
        cols = slice(i * 256, (i + 1) * 256)
        out_ref[:, cols] = (silu_v[i] * scale * ogain_ref[:, cols]).astype(jnp.bfloat16)

    for args in own_sends + query_sends:
        sent(*args)

    def forwards_sent(i, carry):
        forwards(i, lambda copy: copy.wait_send())
        return carry

    lax.fori_loop(0, 16, forwards_sent, 0)

    def output_sent(i, carry):
        sent(*output_send(i // pairs, i % pairs))
        return carry

    lax.fori_loop(0, 8 * pairs, output_sent, 0)


def angle_tables(rows, n_s):
    half = ROPE // 2
    base = THETA ** (-np.arange(half) / half)
    inverse = np.zeros(128)
    inverse[:ROPE] = np.tile(base, 2)

    def both(angles):
        return np.stack([np.cos(angles), np.sin(angles)]).astype(np.float32)

    inner, outer = np.arange(rows), np.arange(n_s) * rows
    return (
        both(inner[:, None] * inverse[None, :]),
        both(outer[:, None] * inverse[None, :])[:, :, None, :],
        both(base[:, None] * inner[None, :]),
        both(outer[:, None] * base[None, :])[:, :, :, None],
    )


def per_device(n_s, n_d, queries, latent, rope_key, latent_gain, kv_weight, gate, out_gain):
    rows, rank = latent.shape
    heads = HEADS // n_d
    pairs = heads // 2
    seq = rows * n_s
    tables = [jnp.asarray(t) for t in angle_tables(rows, n_s)]
    bf = jnp.bfloat16
    dma = pltpu.SemaphoreType.DMA
    vmem = pl.BlockSpec(memory_space=pltpu.VMEM)
    hbm = pl.BlockSpec(memory_space=pl.ANY)
    return pl.pallas_call(
        kernel,
        out_shape=jax.ShapeDtypeStruct(gate.shape, bf),
        in_specs=[hbm, vmem, vmem, vmem, hbm, hbm, vmem, vmem, vmem, vmem, vmem],
        out_specs=vmem,
        scratch_shapes=[
            pltpu.VMEM(kv_weight.shape, bf),
            pltpu.VMEM(queries.shape, bf),
            pltpu.VMEM(gate.shape, bf),
            pltpu.VMEM((16, rows, 256), jnp.float32),
            pltpu.VMEM((rows, rank), bf),
            pltpu.VMEM((ROPE, rows), bf),
            pltpu.VMEM((n_s // 2, 2, rows, rank), bf),
            pltpu.VMEM((n_s // 2, 2, ROPE, rows), bf),
            pltpu.VMEM((n_d, pairs, rows, PAIR), bf),
            pltpu.VMEM((heads, seq, KDIM), bf),
            pltpu.VMEM((heads, seq, 2 * VDIM), bf),
            pltpu.VMEM((n_d, pairs, rows, 2 * VDIM), bf),
            pltpu.VMEM((n_d, pairs, rows, 2 * VDIM), bf),
            dma, dma, dma, dma((2,)),
            dma((16, 5)), dma((16, 2)), dma((16, 5)), dma((16, 2)),
            *[dma((n_d, pairs))] * 4,
        ],
        compiler_params=pltpu.CompilerParams(
            has_side_effects=True, vmem_limit_bytes=60 * 1024 * 1024
        ),
        name="latent_attention",
    )(
        queries, latent, rope_key.T, latent_gain[None, :], kv_weight, gate, out_gain[None, :],
        *tables,
    )


def solution(mesh):
    return jax.shard_map(
        functools.partial(per_device, mesh.shape["sp"], mesh.shape["dp"]),
        mesh=mesh,
        in_specs=(
            P(("dp", "sp"), None),
            P(("dp", "sp"), None),
            P(("dp", "sp"), None),
            P(),
            P(None, "dp"),
            P(("dp", "sp"), None),
            P(),
        ),
        out_specs=P(("dp", "sp"), None),
        check_vma=False,
    )
```

```python
import functools

import jax
import jax.numpy as jnp
import numpy as np
from jax import lax
from jax.experimental import pallas as pl
from jax.experimental.pallas import tpu as pltpu
from jax.sharding import PartitionSpec as P

HEADS = 32
NOPE = 128
ROPE = 64
VDIM = 128
QDIM = NOPE + ROPE
PAIR = 2 * QDIM
KDIM = 256
CHUNK = 1024

EPS = 1e-06
THETA = 10000.0
LOG2E = 1.4426950408889634

MESH = pl.DeviceIdType.MESH
DN_T = (((1,), (1,)), ((), ()))

ORDER = (
    (0, 0), (1, 0), (3, 0), (0, 3), (0, 1), (2, 0), (1, 3), (1, 1),
    (3, 1), (3, 3), (0, 2), (2, 1), (2, 3), (1, 2), (3, 2), (2, 2),
)
WHOLE = (
    (0, 0), (3, 0), (0, 3), (1, 0), (0, 1), (1, 1), (1, 3), (3, 1),
    (3, 3), (0, 2), (2, 0), (2, 1), (1, 2), (2, 3), (3, 2), (2, 2),
)
DONE = (0, 1, 1, 1, 3, 5, 5, 5, 6, 8, 9, 11, 11, 11, 13, 15, 16)
PIECES = ((0, 48), (48, 48), (96, 32))
QUERIES_AT = (4, 9, 13, 16)


def turn(x, cosine, sine, mask):
    partner = jnp.where(mask, pltpu.roll(x, 96, 1), pltpu.roll(x, 32, 1))
    return x * cosine + partner * sine


def kernel(
    q_ref, lat_ref, rk_ref, lgain_ref, w_ref, gate_ref, ogain_ref, ta_ref, tb_ref, ka_ref,
    out_ref,
    w_v, q_v, gate_v, silu_v, own_lat, own_rk, latb, rkb, qb, kbuf, vbuf, ob, orecv,
    w_sem, q_sem, gate_sem, out_sem, own_send, lat_send, lat_recv, rk_send, rk_recv,
    q_send, q_recv, o_send, o_recv,
):
    s, d = lax.axis_index("sp"), lax.axis_index("dp")
    rows = lat_ref.shape[0]
    z, y = s // 4, s % 4
    x, c = d // 2, d % 2
    k, par = z // 2, z % 2
    m = par * 4 + y
    seq = 2 * ((y + 4 - par) % 4) + par
    home = c * 4 + (x + c) % 4
    pairs = 2

    def send(src, dst, ssem, rsem, ts, td):
        same = (ts == s) & (td == d)

        @pl.when(jnp.logical_not(same))
        def _():
            pltpu.make_async_remote_copy(
                src, dst, ssem, rsem, device_id={"sp": ts, "dp": td}, device_id_type=MESH
            ).start()

        @pl.when(same)
        def _():
            pltpu.make_async_copy(src, dst, rsem).start()

    def sent(src, dst, ssem, rsem, ts, td):
        same = (ts == s) & (td == d)

        @pl.when(jnp.logical_not(same))
        def _():
            pltpu.make_async_remote_copy(
                src, dst, ssem, rsem, device_id={"sp": ts, "dp": td}, device_id_type=MESH
            ).wait_send()

    def arrived(dst, rsem):
        pltpu.make_async_copy(dst, dst, rsem).wait()

    def piece(n):
        return pl.ds(*PIECES[n])

    column = (x + y + 2 * c) % 4
    first_block = k * 4 + column
    first_to = ((2 * k + c) * 4 + (x + c) % 4, 2 * column + par)
    root_x = (y + 4 - par) % 4
    root_from = ((2 * k + c) * 4 + (x + 4 - root_x + 2 * par) % 4, seq)
    peers = [
        (s, 2 * ((x + 1) % 4) + c), (s, 2 * ((x + 3) % 4) + c), (s, 2 * x + 1 - c),
        (((z + 2) % 8) * 4 + y, d), (((z + 6) % 8) * 4 + y, d), first_to, root_from,
        *[(k * 8 + home, jnp.int32(t)) for t in range(8)], *[(k * 8 + j, seq) for j in range(8)],
    ]
    barrier = pltpu.get_barrier_semaphore()
    others = jnp.int32(0)
    for ts, td in peers:
        same = (ts == s) & (td == d)

        @pl.when(jnp.logical_not(same))
        def _():
            pl.semaphore_signal(
                barrier, inc=1, device_id={"sp": ts, "dp": td}, device_id_type=MESH
            )

        others = others + jnp.where(same, 0, 1)

    w_copy = pltpu.make_async_copy(w_ref, w_v, w_sem)
    q_copy = pltpu.make_async_copy(q_ref, q_v, q_sem)
    gate_copy = pltpu.make_async_copy(gate_ref, gate_v, gate_sem)
    q_copy.start()
    w_copy.start()
    gate_copy.start()

    wide = lat_ref[...].astype(jnp.float32)
    scale = lax.rsqrt(jnp.mean(wide * wide, axis=-1, keepdims=True) + EPS)
    own_lat[...] = (wide * scale * lgain_ref[...]).astype(jnp.bfloat16)
    half = ROPE // 2
    kca, ksa = ka_ref[0], ka_ref[1]
    kcb, ksb = tb_ref[0, s][:, :half].T, tb_ref[1, s][:, :half].T
    kc, ks = kca * kcb - ksa * ksb, ksa * kcb + kca * ksb
    raw = rk_ref[...].astype(jnp.float32)
    u1, u2 = raw[:half], raw[half:]
    own_rk[:half] = (u1 * kc - u2 * ks).astype(jnp.bfloat16)
    own_rk[half:] = (u2 * kc + u1 * ks).astype(jnp.bfloat16)

    pl.semaphore_wait(barrier, others)
    own_sends = [
        (
            own_lat.at[piece(n)], latb.at[first_block, par, piece(n)], own_send.at[n],
            lat_recv.at[first_block, par, n], *first_to,
        )
        for n in range(len(PIECES))
    ] + [
        (own_rk, rkb.at[first_block, par], own_send.at[len(PIECES)], rk_recv.at[first_block, par], *first_to),
    ]
    for args in own_sends:
        send(*args)

    ones = jnp.ones((rows, 128), jnp.bfloat16)

    def ones_step(i, carry):
        at = pl.ds(pl.multiple_of(i * rows, rows), rows)
        for h in range(4):
            vbuf[h, at, VDIM:] = ones
        return carry

    lax.fori_loop(0, vbuf.shape[1] // rows, ones_step, 0)

    lane = lax.broadcasted_iota(jnp.int32, (rows, 128), 1)
    mask = (lane % 64) < 32
    sign = jnp.where(mask, -1.0, 1.0).astype(jnp.float32)
    ca, sa, cb, sb = ta_ref[0], ta_ref[1], tb_ref[0, s], tb_ref[1, s]
    cosine, sine = ca * cb - sa * sb, (sa * cb + ca * sb) * sign
    cosine_high, sine_high = pltpu.roll(cosine, 64, 1), pltpu.roll(sine, 64, 1)
    q_copy.wait()
    for i in range(HEADS // 2):
        at = slice(i * PAIR + 128, i * PAIR + 256)
        q_v[:, at] = turn(q_v[:, at].astype(jnp.float32), cosine, sine, mask).astype(jnp.bfloat16)
        at = slice(i * PAIR + 256, i * PAIR + 384)
        q_v[:, at] = turn(
            q_v[:, at].astype(jnp.float32), cosine_high, sine_high, mask
        ).astype(jnp.bfloat16)

    def query_sends(turn):
        sends = []
        for p in range(pairs):
            for core in range(2):
                t = 2 * ((x + m // 2 + 4 - turn) % 4) + core
                cols = pl.ds(pl.multiple_of((t * pairs + p) * PAIR, PAIR), PAIR)
                sends.append((
                    q_v.at[:, cols], qb.at[m, p],
                    q_send.at[2 * turn + core, p], q_recv.at[m, p], k * 8 + home, t,
                ))
        return sends

    gate_copy.wait()
    for i in range(16):
        at = slice(i * 256, (i + 1) * 256)
        g = gate_v[:, at].astype(jnp.float32)
        silu_v[i] = g / (1.0 + jnp.exp(-g))
    w_copy.wait()

    low = lax.broadcasted_iota(jnp.int32, (2 * rows, 128), 1) < 64

    def place(i, order=ORDER):
        dk, dx = jnp.int32(0), jnp.int32(0)
        for n, (a, b) in enumerate(order):
            dk = jnp.where(i == n, a, dk)
            dx = jnp.where(i == n, b, dx)
        return dk, dx

    def block_at(dk, dx):
        return ((k + dk) % 4) * 4 + (x + dx) % 4

    last = len(PIECES) - 1

    def part_place(i, part):
        first, second = place(i)
        return (second, first) if part == last else (first, second)

    def forwards(i, part, act):
        first, second = place(i)
        block = block_at(*part_place(i, part))
        own = second == 0
        ahead = own | ((second == 3) & (first < 2))
        back = own | ((second == 1) & (first >= 2))
        ahead_first = own & ((first == 0) | ((first == 3) & (c == 0)))
        back_first = own & ((first == 0) | ((first == 1) & (c == 1)))
        along_x, along_z = (ahead, back), (ahead_first, back_first)
        if part == last:
            along_x, along_z = along_z, along_x
        ways = (
            (along_x[0], s, 2 * ((x + 1) % 4) + c),
            (along_x[1], s, 2 * ((x + 3) % 4) + c),
            (along_z[0], ((z + 2) % 8) * 4 + y, d),
            (along_z[1], ((z + 6) % 8) * 4 + y, d),
            (None, s, 2 * x + 1 - c),
        )
        blocks = [(latb.at[block, c, piece(part)], lat_send.at[i, part], lat_recv.at[block, c, part])]
        if part == 0:
            blocks.append((rkb.at[block, c], rk_send.at[i], rk_recv.at[block, c]))
        for n, (when, ts, td) in enumerate(ways):
            def go(n=n, ts=ts, td=td):
                for buf, ssem, rsem in blocks:
                    act(pltpu.make_async_remote_copy(
                        buf, buf, ssem.at[n], rsem,
                        device_id={"sp": ts, "dp": td}, device_id_type=MESH,
                    ))

            if when is None:
                go()
            else:
                pl.when(when)(go)

    def landed(block, core):
        for n in range(len(PIECES)):
            arrived(latb.at[block, core, piece(n)], lat_recv.at[block, core, n])
        arrived(rkb.at[block, core], rk_recv.at[block, core])

    def send_queries(i):
        for turn in range(4):
            @pl.when(i == QUERIES_AT[turn])
            def _():
                for args in query_sends(turn):
                    send(*args)

    def take(i):
        for n in range(len(PIECES)):
            block = block_at(*part_place(i, n))
            arrived(latb.at[block, c, piece(n)], lat_recv.at[block, c, n])
            if n == 0:
                arrived(rkb.at[block, c], rk_recv.at[block, c])
            forwards(i, n, lambda copy: copy.start())

    def key_step(i, carry):
        @pl.when(i < 16)
        def _():
            take(i)

        send_queries(i)
        start, stop = jnp.int32(0), jnp.int32(0)
        for n in range(1, len(DONE)):
            start = jnp.where(i == n, DONE[n - 1], start)
            stop = jnp.where(i == n, DONE[n], stop)
        return lax.fori_loop(start, stop, whole_step, carry)

    def whole_step(i, carry):
        block = block_at(*place(i, WHOLE))
        landed(block, 1 - c)
        at = pl.ds(pl.multiple_of(i * 2 * rows, 2 * rows), 2 * rows)
        normed = latb[block].reshape(2 * rows, lat_ref.shape[1])
        both_rk = jnp.concatenate([rkb[block, 0], rkb[block, 1]], axis=1).astype(jnp.float32)
        rot = jnp.concatenate([both_rk, jnp.zeros_like(both_rk)], axis=0).T
        rot_high = pltpu.roll(rot, 64, 1)
        for h in range(4):
            both = jnp.dot(
                normed, w_v[:, h * 256 : (h + 1) * 256], preferred_element_type=jnp.float32
            )
            plain = both[:, :NOPE]
            if h % 2 == 0:
                first, second = plain, rot
            else:
                moved = pltpu.roll(plain, 64, 1)
                first = jnp.where(low, 0.0, moved)
                second = jnp.where(low, moved, rot_high)
            kbuf[h, at, :128] = first.astype(jnp.bfloat16)
            kbuf[h, at, 128:] = second.astype(jnp.bfloat16)
            vbuf[h, at, :VDIM] = both[:, NOPE:].astype(jnp.bfloat16)
        return carry

    take(jnp.int32(0))
    lax.fori_loop(1, len(DONE), key_step, 0)

    factor = LOG2E * QDIM ** -0.5
    n_chunks = kbuf.shape[1] // CHUNK

    def output_send(j, p):
        return (ob.at[j, p], orecv.at[d, p], o_send.at[j, p], o_recv.at[d, p], k * 8 + j, seq)

    def query_step(i, carry):
        r, p = (i // pairs + x + 4 - root_x) % 4, i % pairs
        for part in range(2):
            arrived(qb.at[2 * r + part, p], q_recv.at[2 * r + part, p])
        for odd in range(2):
            h = 2 * p + odd
            at = slice(odd * 128, odd * 128 + KDIM)
            q = jnp.concatenate([qb[2 * r, p, :, at], qb[2 * r + 1, p, :, at]], axis=0)

            def score(j):
                return lax.dot_general(
                    q, kbuf[h, j * CHUNK : (j + 1) * CHUNK], DN_T, preferred_element_type=jnp.float32
                )

            following = score(0)
            for j in range(n_chunks):
                scores = following
                if j + 1 < n_chunks:
                    following = score(j + 1)
                top = jnp.max(scores, axis=-1, keepdims=True)
                if j:
                    top = jnp.maximum(top, before)
                raised = jnp.exp2((scores - top) * factor).astype(jnp.bfloat16)
                part_total = jnp.dot(
                    raised, vbuf[h, j * CHUNK : (j + 1) * CHUNK], preferred_element_type=jnp.float32
                )
                total = total * jnp.exp2((before - top) * factor) + part_total if j else part_total
                before = top
            result = (total[:, :VDIM] / total[:, VDIM:]).astype(jnp.bfloat16)
            at = slice(odd * VDIM, (odd + 1) * VDIM)
            ob[2 * r, p, :, at] = result[:rows]
            ob[2 * r + 1, p, :, at] = result[rows:]
        send(*output_send(2 * r, p))
        send(*output_send(2 * r + 1, p))
        return carry

    lax.fori_loop(0, 4 * pairs, query_step, 0)

    for args in sum(map(query_sends, range(4)), own_sends):
        sent(*args)

    def forwards_sent(i, carry):
        for n in range(len(PIECES)):
            forwards(i, n, lambda copy: copy.wait_send())
        return carry

    lax.fori_loop(0, 16, forwards_sent, 0)

    square = jnp.zeros((rows, 1), jnp.float32)
    for p in range(pairs):
        for t in range(8):
            arrived(orecv.at[t, p], o_recv.at[t, p])
            gated = orecv[t, p].astype(jnp.float32) * silu_v[t * pairs + p]
            silu_v[t * pairs + p] = gated
            square = square + jnp.sum(gated * gated, axis=-1, keepdims=True)
    scale = lax.rsqrt(square / (HEADS * VDIM) + EPS)
    outs = []
    for i in range(16):
        cols = slice(i * 256, (i + 1) * 256)
        gate_v[:, cols] = (silu_v[i] * scale * ogain_ref[:, cols]).astype(jnp.bfloat16)
        if i % 4 == 3:
            cols = pl.ds(i // 4 * 1024, 1024)
            outs.append(
                pltpu.make_async_copy(gate_v.at[:, cols], out_ref.at[:, cols], out_sem.at[i // 4])
            )
            outs[-1].start()

    def output_sent(i, carry):
        sent(*output_send(i // pairs, i % pairs))
        return carry

    lax.fori_loop(0, 8 * pairs, output_sent, 0)
    for copy in outs:
        copy.wait()


def angle_tables(rows, n_s):
    half = ROPE // 2
    base = THETA ** (-np.arange(half) / half)
    inverse = np.zeros(128)
    inverse[:ROPE] = np.tile(base, 2)

    def both(angles):
        return np.stack([np.cos(angles), np.sin(angles)]).astype(np.float32)

    inner, outer = np.arange(rows), np.arange(n_s) * rows
    return (
        both(inner[:, None] * inverse[None, :]),
        both(outer[:, None] * inverse[None, :])[:, :, None, :],
        both(base[:, None] * inner[None, :]),
    )


def per_device(n_s, n_d, queries, latent, rope_key, latent_gain, kv_weight, gate, out_gain):
    rows, rank = latent.shape
    heads = HEADS // n_d
    pairs = heads // 2
    seq = rows * n_s
    tables = [jnp.asarray(t) for t in angle_tables(rows, n_s)]
    bf = jnp.bfloat16
    dma = pltpu.SemaphoreType.DMA
    vmem = pl.BlockSpec(memory_space=pltpu.VMEM)
    hbm = pl.BlockSpec(memory_space=pl.ANY)
    return pl.pallas_call(
        kernel,
        out_shape=jax.ShapeDtypeStruct(gate.shape, bf),
        in_specs=[hbm, vmem, vmem, vmem, hbm, hbm, vmem, vmem, vmem, vmem],
        out_specs=hbm,
        scratch_shapes=[
            pltpu.VMEM(kv_weight.shape, bf),
            pltpu.VMEM(queries.shape, bf),
            pltpu.VMEM(gate.shape, bf),
            pltpu.VMEM((16, rows, 256), jnp.float32),
            pltpu.VMEM((rows, rank), bf),
            pltpu.VMEM((ROPE, rows), bf),
            pltpu.VMEM((n_s // 2, 2, rows, rank), bf),
            pltpu.VMEM((n_s // 2, 2, ROPE, rows), bf),
            pltpu.VMEM((n_d, pairs, rows, PAIR), bf),
            pltpu.VMEM((heads, seq, KDIM), bf),
            pltpu.VMEM((heads, seq, 2 * VDIM), bf),
            pltpu.VMEM((n_d, pairs, rows, 2 * VDIM), bf),
            pltpu.VMEM((n_d, pairs, rows, 2 * VDIM), bf),
            dma, dma, dma, dma((4,)), dma((len(PIECES) + 1,)),
            dma((16, len(PIECES), 5)), dma((16, 2, len(PIECES))), dma((16, 5)), dma((16, 2)),
            *[dma((n_d, pairs))] * 4,
        ],
        compiler_params=pltpu.CompilerParams(
            has_side_effects=True, collective_id=0, vmem_limit_bytes=60 * 1024 * 1024
        ),
        name="latent_attention",
    )(
        queries, latent, rope_key.T, latent_gain[None, :], kv_weight, gate, out_gain[None, :],
        *tables,
    )


def solution(mesh):
    return jax.shard_map(
        functools.partial(per_device, mesh.shape["sp"], mesh.shape["dp"]),
        mesh=mesh,
        in_specs=(
            P(("dp", "sp"), None),
            P(("dp", "sp"), None),
            P(("dp", "sp"), None),
            P(),
            P(None, "dp"),
            P(("dp", "sp"), None),
            P(),
        ),
        out_specs=P(("dp", "sp"), None),
        check_vma=False,
    )
```

```python
import functools

import jax
import jax.numpy as jnp
import numpy as np
from jax import lax
from jax.experimental import pallas as pl
from jax.experimental.pallas import tpu as pltpu
from jax.sharding import PartitionSpec as P

HEADS = 32
NOPE = 128
ROPE = 64
VDIM = 128
QDIM = NOPE + ROPE
PAIR = 2 * QDIM
KDIM = 256
CHUNK = 1024

EPS = 1e-06
THETA = 10000.0
LOG2E = 1.4426950408889634

MESH = pl.DeviceIdType.MESH
DN_T = (((1,), (1,)), ((), ()))

ORDER = (
    (0, 0), (1, 0), (3, 0), (0, 3), (0, 1), (2, 0), (1, 3), (1, 1),
    (3, 1), (3, 3), (0, 2), (2, 1), (2, 3), (1, 2), (3, 2), (2, 2),
)
WHOLE = (
    (0, 0), (3, 0), (0, 3), (1, 0), (0, 1), (1, 1), (1, 3), (3, 1),
    (3, 3), (0, 2), (2, 0), (2, 1), (1, 2), (2, 3), (3, 2), (2, 2),
)
DONE = (0, 1, 1, 1, 3, 5, 5, 5, 6, 8, 9, 11, 11, 11, 13, 15, 16)
PIECES = ((0, 48), (48, 48), (96, 32))
QUERIES_AT = (0, 4, 8, 12)


def turn(x, cosine, sine, mask):
    partner = jnp.where(mask, pltpu.roll(x, 96, 1), pltpu.roll(x, 32, 1))
    return x * cosine + partner * sine


def kernel(
    q_ref, lat_ref, rk_ref, lgain_ref, w_ref, gate_ref, ogain_ref, ta_ref, tb_ref, ka_ref,
    out_ref,
    w_v, q_v, gate_v, silu_v, own_lat, own_rk, latb, rkb, qb, kbuf, vbuf, ob, orecv,
    w_sem, q_sem, gate_sem, out_sem, own_send, lat_send, lat_recv, rk_send, rk_recv,
    q_send, q_recv, o_send, o_recv,
):
    s, d = lax.axis_index("sp"), lax.axis_index("dp")
    rows = lat_ref.shape[0]
    z, y = s // 4, s % 4
    x, c = d // 2, d % 2
    k, par = z // 2, z % 2
    m = par * 4 + y
    seq = 2 * ((y + 4 - 2 * par) % 4) + par
    home = c * 4 + (x + 2 * c) % 4
    pairs, heads = 2, 4

    def send(src, dst, ssem, rsem, ts, td):
        same = (ts == s) & (td == d)

        @pl.when(jnp.logical_not(same))
        def _():
            pltpu.make_async_remote_copy(
                src, dst, ssem, rsem, device_id={"sp": ts, "dp": td}, device_id_type=MESH
            ).start()

        @pl.when(same)
        def _():
            pltpu.make_async_copy(src, dst, rsem).start()

    def sent(src, dst, ssem, rsem, ts, td):
        same = (ts == s) & (td == d)

        @pl.when(jnp.logical_not(same))
        def _():
            pltpu.make_async_remote_copy(
                src, dst, ssem, rsem, device_id={"sp": ts, "dp": td}, device_id_type=MESH
            ).wait_send()

    def arrived(dst, rsem):
        pltpu.make_async_copy(dst, dst, rsem).wait()

    def piece(n):
        return pl.ds(*PIECES[n])

    column = (x + y + 2 * c) % 4
    first_block = k * 4 + column
    first_to = ((2 * k + c) * 4 + (x + 2 * c) % 4, 2 * column + par)
    root_x = (y + 4 - 2 * par) % 4
    root_from = ((2 * k + c) * 4 + (x + 4 - root_x + 2 * par) % 4, seq)
    peers = [
        (s, 2 * ((x + 1) % 4) + c), (s, 2 * ((x + 3) % 4) + c), (s, 2 * x + 1 - c),
        (((z + 2) % 8) * 4 + y, d), (((z + 6) % 8) * 4 + y, d), first_to, root_from,
        *[(k * 8 + home, jnp.int32(t)) for t in range(8)], *[(k * 8 + j, seq) for j in range(8)],
    ]
    barrier = pltpu.get_barrier_semaphore()
    others = jnp.int32(0)
    for ts, td in peers:
        same = (ts == s) & (td == d)

        @pl.when(jnp.logical_not(same))
        def _():
            pl.semaphore_signal(
                barrier, inc=1, device_id={"sp": ts, "dp": td}, device_id_type=MESH
            )

        others = others + jnp.where(same, 0, 1)

    w_copy = pltpu.make_async_copy(w_ref, w_v, w_sem)
    q_copy = pltpu.make_async_copy(q_ref, q_v, q_sem)
    gate_copy = pltpu.make_async_copy(gate_ref, gate_v, gate_sem)
    q_copy.start()
    w_copy.start()
    gate_copy.start()

    wide = lat_ref[...].astype(jnp.float32)
    scale = lax.rsqrt(jnp.mean(wide * wide, axis=-1, keepdims=True) + EPS)
    own_lat[...] = (wide * scale * lgain_ref[...]).astype(jnp.bfloat16)
    half = ROPE // 2
    kca, ksa = ka_ref[0], ka_ref[1]
    kcb, ksb = tb_ref[0, s][:, :half].T, tb_ref[1, s][:, :half].T
    kc, ks = kca * kcb - ksa * ksb, ksa * kcb + kca * ksb
    raw = rk_ref[...].astype(jnp.float32)
    u1, u2 = raw[:half], raw[half:]
    own_rk[:half] = (u1 * kc - u2 * ks).astype(jnp.bfloat16)
    own_rk[half:] = (u2 * kc + u1 * ks).astype(jnp.bfloat16)

    pl.semaphore_wait(barrier, others)
    own_sends = [
        (
            own_lat.at[piece(n)], latb.at[2 * first_block + par, piece(n)], own_send.at[n],
            lat_recv.at[first_block, par, n], *first_to,
        )
        for n in range(len(PIECES))
    ] + [
        (own_rk, rkb.at[2 * first_block + par], own_send.at[len(PIECES)], rk_recv.at[first_block, par], *first_to),
    ]
    for args in own_sends:
        send(*args)

    ones = jnp.ones((rows, 128), jnp.bfloat16)

    def ones_step(i, carry):
        at = pl.ds(pl.multiple_of(i * rows, rows), rows)
        for h in range(4):
            vbuf[h, at, VDIM:] = ones
        return carry

    lax.fori_loop(0, vbuf.shape[1] // rows, ones_step, 0)

    lane = lax.broadcasted_iota(jnp.int32, (rows, 128), 1)
    mask = (lane % 64) < 32
    sign = jnp.where(mask, -1.0, 1.0).astype(jnp.float32)
    ca, sa, cb, sb = ta_ref[0], ta_ref[1], tb_ref[0, s], tb_ref[1, s]
    cosine, sine = ca * cb - sa * sb, (sa * cb + ca * sb) * sign
    cosine_high, sine_high = pltpu.roll(cosine, 64, 1), pltpu.roll(sine, 64, 1)
    q_copy.wait()
    for i in range(HEADS // 2):
        at = slice(i * PAIR + 128, i * PAIR + 256)
        q_v[:, at] = turn(q_v[:, at].astype(jnp.float32), cosine, sine, mask).astype(jnp.bfloat16)
        at = slice(i * PAIR + 256, i * PAIR + 384)
        q_v[:, at] = turn(
            q_v[:, at].astype(jnp.float32), cosine_high, sine_high, mask
        ).astype(jnp.bfloat16)

    def query_sends(turn):
        sends = []
        for p in range(pairs):
            for core in range(2):
                t = 2 * ((x + m // 2 + 4 - turn) % 4) + core
                cols = pl.ds(pl.multiple_of((t * pairs + p) * PAIR, PAIR), PAIR)
                sends.append((
                    q_v.at[:, cols], qb.at[m, p],
                    q_send.at[2 * turn + core, p], q_recv.at[m, p], k * 8 + home, t,
                ))
        return sends

    gate_copy.wait()
    for i in range(HEADS):
        at = slice(i * VDIM, (i + 1) * VDIM)
        g = gate_v[:, at].astype(jnp.float32)
        silu_v[i] = g / (1.0 + jnp.exp(-g))
    w_copy.wait()

    low = lax.broadcasted_iota(jnp.int32, (2 * rows, 128), 1) < 64

    def place(i, order=ORDER):
        dk, dx = jnp.int32(0), jnp.int32(0)
        for n, (a, b) in enumerate(order):
            dk = jnp.where(i == n, a, dk)
            dx = jnp.where(i == n, b, dx)
        return dk, dx

    def block_at(dk, dx):
        return ((k + dk) % 4) * 4 + (x + dx) % 4

    last = len(PIECES) - 1

    def part_place(i, part):
        first, second = place(i)
        return (second, first) if part == last else (first, second)

    def forwards(i, part):
        first, second = place(i)
        block = block_at(*part_place(i, part))
        own = second == 0
        ahead = own | ((second == 3) & (first < 2))
        back = own | ((second == 1) & (first >= 2))
        ahead_first = own & ((first == 0) | ((first == 3) & (c == 0)))
        back_first = own & ((first == 0) | ((first == 1) & (c == 1)))
        along_x, along_z = (ahead, back), (ahead_first, back_first)
        if part == last:
            along_x, along_z = along_z, along_x
        ways = (
            (along_x[0], s, 2 * ((x + 1) % 4) + c),
            (along_x[1], s, 2 * ((x + 3) % 4) + c),
            (along_z[0], ((z + 2) % 8) * 4 + y, d),
            (along_z[1], ((z + 6) % 8) * 4 + y, d),
            (None, s, 2 * x + 1 - c),
        )
        blocks = [(latb.at[2 * block + c, piece(part)], lat_send, lat_recv.at[block, c, part])]
        if part == 0:
            blocks.append((rkb.at[2 * block + c], rk_send, rk_recv.at[block, c]))
        for when, ts, td in ways:
            def go(ts=ts, td=td):
                for buf, ssem, rsem in blocks:
                    pltpu.make_async_remote_copy(
                        buf, buf, ssem, rsem,
                        device_id={"sp": ts, "dp": td}, device_id_type=MESH,
                    ).start()

            if when is None:
                go()
            else:
                pl.when(when)(go)

    def landed(block, core):
        for n in range(len(PIECES)):
            arrived(latb.at[2 * block + core, piece(n)], lat_recv.at[block, core, n])
        arrived(rkb.at[2 * block + core], rk_recv.at[block, core])

    def send_queries(i):
        for turn in range(4):
            @pl.when(i == QUERIES_AT[turn])
            def _():
                for args in query_sends(turn):
                    send(*args)

    def take(i, part):
        block = block_at(*part_place(i, part))
        arrived(latb.at[2 * block + c, piece(part)], lat_recv.at[block, c, part])
        if part == 0:
            arrived(rkb.at[2 * block + c], rk_recv.at[block, c])
        forwards(i, part)

    def key_step(i, carry):
        @pl.when(i < 16)
        def _():
            for part in range(len(PIECES)):
                take(i, part)

        send_queries(i)
        lax.fori_loop(*between(DONE, i), whole_step, 0)
        return carry

    def between(table, i):
        start, stop = jnp.int32(0), jnp.int32(0)
        for n in range(1, len(table)):
            start = jnp.where(i == n, table[n - 1], start)
            stop = jnp.where(i == n, table[n], stop)
        return start, stop

    factor = LOG2E * QDIM ** -0.5
    n_chunks = kbuf.shape[1] // CHUNK

    def step_place(i):
        return (i // pairs + x + 4 - root_x) % 4, i % pairs

    def attend(i, odd, chunks, total, before):
        r, p = step_place(i)
        h = 2 * p + odd
        at = slice(odd * 128, odd * 128 + KDIM)
        q = jnp.concatenate([qb[2 * r, p, :, at], qb[2 * r + 1, p, :, at]], axis=0)

        def score(j):
            return lax.dot_general(
                q, kbuf[h, j * CHUNK : (j + 1) * CHUNK], DN_T, preferred_element_type=jnp.float32
            )

        following = score(chunks[0])
        for j in chunks:
            scores = following
            if j != chunks[-1]:
                following = score(j + 1)
            top = jnp.max(scores, axis=-1, keepdims=True)
            if before is not None:
                top = jnp.maximum(top, before)
            raised = jnp.exp2((scores - top) * factor).astype(jnp.bfloat16)
            part_total = jnp.dot(
                raised, vbuf[h, j * CHUNK : (j + 1) * CHUNK], preferred_element_type=jnp.float32
            )
            total = part_total if before is None else total * jnp.exp2((before - top) * factor) + part_total
            before = top
        return total, before

    def whole_step(i, carry):
        block = block_at(*place(i, WHOLE))
        landed(block, 1 - c)
        at = pl.ds(pl.multiple_of(i * 2 * rows, 2 * rows), 2 * rows)
        normed = latb[pl.ds(2 * block, 2)].reshape(2 * rows, lat_ref.shape[1])
        both_rk = jnp.concatenate([rkb[2 * block], rkb[2 * block + 1]], axis=1).astype(jnp.float32)
        rot = jnp.concatenate([both_rk, jnp.zeros_like(both_rk)], axis=0).T
        rot_high = pltpu.roll(rot, 64, 1)
        for h in range(4):
            both = jnp.dot(
                normed, w_v[:, h * 256 : (h + 1) * 256], preferred_element_type=jnp.float32
            )
            plain = both[:, :NOPE]
            if h % 2 == 0:
                first, second = plain, rot
            else:
                moved = pltpu.roll(plain, 64, 1)
                first = jnp.where(low, 0.0, moved)
                second = jnp.where(low, moved, rot_high)
            kbuf[h, at, :128] = first.astype(jnp.bfloat16)
            kbuf[h, at, 128:] = second.astype(jnp.bfloat16)
            vbuf[h, at, :VDIM] = both[:, NOPE:].astype(jnp.bfloat16)
        return carry

    for part in range(len(PIECES)):
        take(jnp.int32(0), part)
    send_queries(jnp.int32(0))
    lax.fori_loop(1, len(DONE), key_step, 0)

    def output_send(j, h):
        return (ob.at[j, h], orecv.at[d, h], o_send.at[j, h], o_recv.at[d, h], k * 8 + j, seq)

    def query_step(i, carry, split=False):
        r, p = step_place(i)
        for part in range(2):
            arrived(qb.at[2 * r + part, p], q_recv.at[2 * r + part, p])
        for odd in range(2):
            total, _ = attend(i, odd, range(n_chunks), None, None)
            result = (total[:, :VDIM] / total[:, VDIM:]).astype(jnp.bfloat16)
            ob[2 * r, 2 * p + odd] = result[:rows]
            ob[2 * r + 1, 2 * p + odd] = result[rows:]
            if split or odd:
                for h in (2 * p + odd,) if split else (2 * p, 2 * p + 1):
                    send(*output_send(2 * r, h))
                    send(*output_send(2 * r + 1, h))
        return carry

    lax.fori_loop(0, 4 * pairs - 1, query_step, 0)
    query_step(jnp.int32(4 * pairs - 1), 0, True)

    for args in sum(map(query_sends, range(4)), own_sends):
        sent(*args)

    arrived(latb.at[pl.ds(0, 31)], lat_send)
    arrived(rkb.at[pl.ds(0, 31)], rk_send)

    square = jnp.zeros((rows, 1), jnp.float32)
    for h in range(4):
        for t in range(8):
            arrived(orecv.at[t, h], o_recv.at[t, h])
            gated = orecv[t, h].astype(jnp.float32) * silu_v[t * 4 + h]
            silu_v[t * 4 + h] = gated
            square = square + jnp.sum(gated * gated, axis=-1, keepdims=True)
    scale = lax.rsqrt(square / (HEADS * VDIM) + EPS)
    outs = []
    for i in range(HEADS):
        cols = slice(i * VDIM, (i + 1) * VDIM)
        gate_v[:, cols] = (silu_v[i] * scale * ogain_ref[:, cols]).astype(jnp.bfloat16)
        if i % 8 == 7:
            cols = pl.ds(i // 8 * 1024, 1024)
            outs.append(
                pltpu.make_async_copy(gate_v.at[:, cols], out_ref.at[:, cols], out_sem.at[i // 8])
            )
            outs[-1].start()

    def output_sent(i, carry):
        sent(*output_send(i // heads, i % heads))
        return carry

    lax.fori_loop(0, 8 * heads, output_sent, 0)
    for copy in outs:
        copy.wait()


def angle_tables(rows, n_s):
    half = ROPE // 2
    base = THETA ** (-np.arange(half) / half)
    inverse = np.zeros(128)
    inverse[:ROPE] = np.tile(base, 2)

    def both(angles):
        return np.stack([np.cos(angles), np.sin(angles)]).astype(np.float32)

    inner, outer = np.arange(rows), np.arange(n_s) * rows
    return (
        both(inner[:, None] * inverse[None, :]),
        both(outer[:, None] * inverse[None, :])[:, :, None, :],
        both(base[:, None] * inner[None, :]),
    )


def per_device(n_s, n_d, queries, latent, rope_key, latent_gain, kv_weight, gate, out_gain):
    rows, rank = latent.shape
    heads = HEADS // n_d
    pairs = heads // 2
    seq = rows * n_s
    tables = [jnp.asarray(t) for t in angle_tables(rows, n_s)]
    bf = jnp.bfloat16
    dma = pltpu.SemaphoreType.DMA
    vmem = pl.BlockSpec(memory_space=pltpu.VMEM)
    hbm = pl.BlockSpec(memory_space=pl.ANY)
    return pl.pallas_call(
        kernel,
        out_shape=jax.ShapeDtypeStruct(gate.shape, bf),
        in_specs=[hbm, vmem, vmem, vmem, hbm, hbm, vmem, vmem, vmem, vmem],
        out_specs=hbm,
        scratch_shapes=[
            pltpu.VMEM(kv_weight.shape, bf),
            pltpu.VMEM(queries.shape, bf),
            pltpu.VMEM(gate.shape, bf),
            pltpu.VMEM((HEADS, rows, VDIM), jnp.float32),
            pltpu.VMEM((rows, rank), bf),
            pltpu.VMEM((ROPE, rows), bf),
            pltpu.VMEM((n_s, rows, rank), bf),
            pltpu.VMEM((n_s, ROPE, rows), bf),
            pltpu.VMEM((n_d, pairs, rows, PAIR), bf),
            pltpu.VMEM((heads, seq, KDIM), bf),
            pltpu.VMEM((heads, seq, 2 * VDIM), bf),
            pltpu.VMEM((n_d, heads, rows, VDIM), bf),
            pltpu.VMEM((n_d, heads, rows, VDIM), bf),
            dma, dma, dma, dma((4,)), dma((len(PIECES) + 1,)),
            dma, dma((16, 2, len(PIECES))), dma, dma((16, 2)),
            *[dma((n_d, pairs))] * 2, *[dma((n_d, heads))] * 2,
        ],
        compiler_params=pltpu.CompilerParams(
            has_side_effects=True, collective_id=0, vmem_limit_bytes=60 * 1024 * 1024
        ),
        name="latent_attention",
    )(
        queries, latent, rope_key.T, latent_gain[None, :], kv_weight, gate, out_gain[None, :],
        *tables,
    )


def solution(mesh):
    return jax.shard_map(
        functools.partial(per_device, mesh.shape["sp"], mesh.shape["dp"]),
        mesh=mesh,
        in_specs=(
            P(("dp", "sp"), None),
            P(("dp", "sp"), None),
            P(("dp", "sp"), None),
            P(),
            P(None, "dp"),
            P(("dp", "sp"), None),
            P(),
        ),
        out_specs=P(("dp", "sp"), None),
        check_vma=False,
    )
```

```python
import functools

import jax
import jax.numpy as jnp
import numpy as np
from jax import lax
from jax.experimental import pallas as pl
from jax.experimental.pallas import tpu as pltpu
from jax.sharding import PartitionSpec as P

HEADS = 32
NOPE = 128
ROPE = 64
VDIM = 128
QDIM = NOPE + ROPE
PAIR = 2 * QDIM
KDIM = 256
CHUNK = 1024

EPS = 1e-06
THETA = 10000.0
LOG2E = 1.4426950408889634

MESH = pl.DeviceIdType.MESH
DN_T = (((1,), (1,)), ((), ()))

ORDER = (
    (0, 0), (1, 0), (3, 0), (0, 3), (0, 1), (2, 0), (1, 3), (1, 1),
    (3, 1), (3, 3), (0, 2), (2, 1), (2, 3), (1, 2), (3, 2), (2, 2),
)
WHOLE = (
    (0, 0), (3, 0), (0, 3), (1, 0), (0, 1), (1, 1), (1, 3), (3, 1),
    (3, 3), (0, 2), (2, 0), (2, 1), (1, 2), (2, 3), (3, 2), (2, 2),
)
DONE = (0, 1, 1, 1, 3, 5, 5, 5, 6, 8, 9, 11, 11, 11, 15, 16)
PIECES = ((0, 48), (48, 48), (96, 32))
QUERIES_AT = (0, 3, 7, 15)


def turn(x, cosine, sine, mask):
    partner = jnp.where(mask, pltpu.roll(x, 96, 1), pltpu.roll(x, 32, 1))
    return x * cosine + partner * sine


def kernel(
    q_ref, lat_ref, rk_ref, lgain_ref, w_ref, gate_ref, ogain_ref, ta_ref, tb_ref, ka_ref,
    out_ref,
    w_v, q_v, gate_v, silu_v, own_lat, own_rk, latb, rkb, qb, kbuf, vbuf, ob, orecv,
    w_sem, q_sem, gate_sem, out_sem, own_send, lat_send, lat_recv, partner_recv, rk_send, rk_recv,
    q_send, q_recv, o_send, o_recv,
):
    s, d = lax.axis_index("sp"), lax.axis_index("dp")
    rows = lat_ref.shape[0]
    z, y = s // 4, s % 4
    x, c = d // 2, d % 2
    k, par = z // 2, z % 2
    m = par * 4 + y
    seq = 2 * ((y + 4 - 2 * par) % 4) + par
    home = c * 4 + (x + 2 * c) % 4
    pairs, heads = 2, 4

    def send(src, dst, ssem, rsem, ts, td):
        same = (ts == s) & (td == d)

        @pl.when(jnp.logical_not(same))
        def _():
            pltpu.make_async_remote_copy(
                src, dst, ssem, rsem, device_id={"sp": ts, "dp": td}, device_id_type=MESH
            ).start()

        @pl.when(same)
        def _():
            pltpu.make_async_copy(src, dst, rsem).start()

    def sent(src, dst, ssem, rsem, ts, td):
        same = (ts == s) & (td == d)

        @pl.when(jnp.logical_not(same))
        def _():
            pltpu.make_async_remote_copy(
                src, dst, ssem, rsem, device_id={"sp": ts, "dp": td}, device_id_type=MESH
            ).wait_send()

    def arrived(dst, rsem):
        pltpu.make_async_copy(dst, dst, rsem).wait()

    def piece(n):
        return pl.ds(*PIECES[n])

    column = (x + y + 2 * c) % 4
    first_block = k * 4 + column
    first_to = ((2 * k + c) * 4 + (x + 2 * c) % 4, 2 * column + par)
    root_x = (y + 4 - 2 * par) % 4
    root_from = ((2 * k + c) * 4 + (x + 4 - root_x + 2 * par) % 4, seq)
    peers = [
        (s, 2 * ((x + 1) % 4) + c), (s, 2 * ((x + 3) % 4) + c), (s, 2 * x + 1 - c),
        (((z + 2) % 8) * 4 + y, d), (((z + 6) % 8) * 4 + y, d), first_to, root_from,
        *[(k * 8 + home, jnp.int32(t)) for t in range(8)], *[(k * 8 + j, seq) for j in range(8)],
    ]
    barrier = pltpu.get_barrier_semaphore()
    others = jnp.int32(0)
    for ts, td in peers:
        same = (ts == s) & (td == d)

        @pl.when(jnp.logical_not(same))
        def _():
            pl.semaphore_signal(
                barrier, inc=1, device_id={"sp": ts, "dp": td}, device_id_type=MESH
            )

        others = others + jnp.where(same, 0, 1)

    w_copy = pltpu.make_async_copy(w_ref, w_v, w_sem)
    q_copy = pltpu.make_async_copy(q_ref, q_v, q_sem)
    gate_copy = pltpu.make_async_copy(gate_ref, gate_v, gate_sem)
    q_copy.start()
    w_copy.start()
    gate_copy.start()

    wide = lat_ref[...].astype(jnp.float32)
    scale = lax.rsqrt(jnp.mean(wide * wide, axis=-1, keepdims=True) + EPS)
    own_lat[...] = (wide * scale * lgain_ref[...]).astype(jnp.bfloat16)
    half = ROPE // 2
    kca, ksa = ka_ref[0], ka_ref[1]
    kcb, ksb = tb_ref[0, s][:, :half].T, tb_ref[1, s][:, :half].T
    kc, ks = kca * kcb - ksa * ksb, ksa * kcb + kca * ksb
    raw = rk_ref[...].astype(jnp.float32)
    u1, u2 = raw[:half], raw[half:]
    own_rk[:half] = (u1 * kc - u2 * ks).astype(jnp.bfloat16)
    own_rk[half:] = (u2 * kc + u1 * ks).astype(jnp.bfloat16)

    pl.semaphore_wait(barrier, others)
    own_sends = [
        (
            own_lat.at[piece(n)], latb.at[2 * first_block + par, piece(n)], own_send.at[n],
            lat_recv.at[first_block, n], *first_to,
        )
        for n in range(len(PIECES))
    ] + [
        (own_rk, rkb.at[2 * first_block + par], own_send.at[len(PIECES)], rk_recv.at[first_block, par], *first_to),
    ]
    for args in own_sends:
        send(*args)

    ones = jnp.ones((rows, 128), jnp.bfloat16)

    def ones_step(i, carry):
        at = pl.ds(pl.multiple_of(i * rows, rows), rows)
        for h in range(4):
            vbuf[h, at, VDIM:] = ones
        return carry

    lax.fori_loop(0, vbuf.shape[1] // rows, ones_step, 0)

    lane = lax.broadcasted_iota(jnp.int32, (rows, 128), 1)
    mask = (lane % 64) < 32
    sign = jnp.where(mask, -1.0, 1.0).astype(jnp.float32)
    ca, sa, cb, sb = ta_ref[0], ta_ref[1], tb_ref[0, s], tb_ref[1, s]
    cosine, sine = ca * cb - sa * sb, (sa * cb + ca * sb) * sign
    cosine_high, sine_high = pltpu.roll(cosine, 64, 1), pltpu.roll(sine, 64, 1)
    q_copy.wait()
    for i in range(HEADS // 2):
        at = slice(i * PAIR + 128, i * PAIR + 256)
        q_v[:, at] = turn(q_v[:, at].astype(jnp.float32), cosine, sine, mask).astype(jnp.bfloat16)
        at = slice(i * PAIR + 256, i * PAIR + 384)
        q_v[:, at] = turn(
            q_v[:, at].astype(jnp.float32), cosine_high, sine_high, mask
        ).astype(jnp.bfloat16)

    def query_sends(turn):
        sends = []
        for p in range(pairs):
            for core in range(2):
                t = 2 * ((x + m // 2 + 4 - turn) % 4) + core
                cols = pl.ds(pl.multiple_of((t * pairs + p) * PAIR, PAIR), PAIR)
                sends.append((
                    q_v.at[:, cols], qb.at[m, p],
                    q_send, q_recv.at[m, p], k * 8 + home, t,
                ))
        return sends

    gate_copy.wait()
    for i in range(HEADS):
        at = slice(i * VDIM, (i + 1) * VDIM)
        g = gate_v[:, at].astype(jnp.float32)
        silu_v[i] = g / (1.0 + jnp.exp(-g))
    w_copy.wait()

    low = lax.broadcasted_iota(jnp.int32, (2 * rows, 128), 1) < 64

    def place(i, order=ORDER):
        dk, dx = jnp.int32(0), jnp.int32(0)
        for n, (a, b) in enumerate(order):
            dk = jnp.where(i == n, a, dk)
            dx = jnp.where(i == n, b, dx)
        return dk, dx

    def block_at(dk, dx):
        return ((k + dk) % 4) * 4 + (x + dx) % 4

    last = len(PIECES) - 1

    def part_place(i, part):
        first, second = place(i)
        return (second, first) if part == last else (first, second)

    def forwards(i, part):
        first, second = place(i)
        block = block_at(*part_place(i, part))
        own = second == 0
        ahead = own | ((second == 3) & (first < 2))
        back = own | ((second == 1) & (first >= 2))
        ahead_first = own & ((first == 0) | ((first == 3) & (c == 0)))
        back_first = own & ((first == 0) | ((first == 1) & (c == 1)))
        along_x, along_z = (ahead, back), (ahead_first, back_first)
        if part == last:
            along_x, along_z = along_z, along_x
        ways = (
            (along_x[0], s, 2 * ((x + 1) % 4) + c),
            (along_x[1], s, 2 * ((x + 3) % 4) + c),
            (along_z[0], ((z + 2) % 8) * 4 + y, d),
            (along_z[1], ((z + 6) % 8) * 4 + y, d),
            (None, s, 2 * x + 1 - c),
        )
        blocks = [(latb.at[2 * block + c, piece(part)], lat_send, lat_recv.at[block, part])]
        if part == 0:
            blocks.append((rkb.at[2 * block + c], rk_send, rk_recv.at[block, c]))
        for when, ts, td in ways:
            def go(ts=ts, td=td, when=when):
                for buf, ssem, rsem in blocks:
                    if when is None and ssem is lat_send:
                        rsem = partner_recv.at[block]
                    pltpu.make_async_remote_copy(
                        buf, buf, ssem, rsem,
                        device_id={"sp": ts, "dp": td}, device_id_type=MESH,
                    ).start()

            if when is None:
                go()
            else:
                pl.when(when)(go)

    def landed(block, core):
        arrived(latb.at[2 * block + core], partner_recv.at[block])
        arrived(rkb.at[2 * block + core], rk_recv.at[block, core])

    def send_queries(i):
        for turn in range(4):
            @pl.when(i == QUERIES_AT[turn])
            def _():
                for args in query_sends(turn):
                    send(*args)

    def take(i, part):
        block = block_at(*part_place(i, part))
        arrived(latb.at[2 * block + c, piece(part)], lat_recv.at[block, part])
        if part == 0:
            arrived(rkb.at[2 * block + c], rk_recv.at[block, c])
        forwards(i, part)

    def key_step(i, carry):
        for part in range(len(PIECES)):
            take(i, part)
        send_queries(i)
        lax.fori_loop(*between(DONE, i), whole_step, 0)
        return carry

    def between(table, i):
        start, stop = jnp.int32(0), jnp.int32(0)
        for n in range(1, len(table)):
            start = jnp.where(i == n, table[n - 1], start)
            stop = jnp.where(i == n, table[n], stop)
        return start, stop

    factor = LOG2E * QDIM ** -0.5
    n_chunks = kbuf.shape[1] // CHUNK

    def step_place(i):
        return (i // pairs + x + 4 - root_x) % 4, i % pairs

    def attend(i, odd, chunks, total, before):
        r, p = step_place(i)
        h = 2 * p + odd
        at = slice(odd * 128, odd * 128 + KDIM)
        q = jnp.concatenate([qb[2 * r, p, :, at], qb[2 * r + 1, p, :, at]], axis=0)

        def score(j):
            return lax.dot_general(
                q, kbuf[h, j * CHUNK : (j + 1) * CHUNK], DN_T, preferred_element_type=jnp.float32
            )

        following = score(chunks[0])
        for j in chunks:
            scores = following
            if j != chunks[-1]:
                following = score(j + 1)
            top = jnp.max(scores, axis=-1, keepdims=True)
            if before is not None:
                top = jnp.maximum(top, before)
            raised = jnp.exp2((scores - top) * factor).astype(jnp.bfloat16)
            part_total = jnp.dot(
                raised, vbuf[h, j * CHUNK : (j + 1) * CHUNK], preferred_element_type=jnp.float32
            )
            total = part_total if before is None else total * jnp.exp2((before - top) * factor) + part_total
            before = top
        return total, before

    def whole_step(i, carry):
        block = block_at(*place(i, WHOLE))
        landed(block, 1 - c)
        at = pl.ds(pl.multiple_of(i * 2 * rows, 2 * rows), 2 * rows)
        normed = latb[pl.ds(2 * block, 2)].reshape(2 * rows, lat_ref.shape[1])
        both_rk = jnp.concatenate([rkb[2 * block], rkb[2 * block + 1]], axis=1).astype(jnp.float32)
        rot = jnp.concatenate([both_rk, jnp.zeros_like(both_rk)], axis=0).T
        rot_high = pltpu.roll(rot, 64, 1)
        for h in range(4):
            both = jnp.dot(
                normed, w_v[:, h * 256 : (h + 1) * 256], preferred_element_type=jnp.float32
            )
            plain = both[:, :NOPE]
            if h % 2 == 0:
                first, second = plain, rot
            else:
                moved = pltpu.roll(plain, 64, 1)
                first = jnp.where(low, 0.0, moved)
                second = jnp.where(low, moved, rot_high)
            kbuf[h, at, :128] = first.astype(jnp.bfloat16)
            kbuf[h, at, 128:] = second.astype(jnp.bfloat16)
            vbuf[h, at, :VDIM] = both[:, NOPE:].astype(jnp.bfloat16)
        return carry

    for part in range(len(PIECES)):
        take(jnp.int32(0), part)
    send_queries(jnp.int32(0))
    lax.fori_loop(1, len(DONE), key_step, 0)

    def output_send(j, h):
        return (ob.at[j, h], orecv.at[d, h], o_send, o_recv.at[d, h], k * 8 + j, seq)

    def query_step(i, carry, split=False):
        r, p = step_place(i)
        for part in range(2):
            arrived(qb.at[2 * r + part, p], q_recv.at[2 * r + part, p])
        for odd in range(2):
            total, _ = attend(i, odd, range(n_chunks), None, None)
            result = (total[:, :VDIM] / total[:, VDIM:]).astype(jnp.bfloat16)
            ob[2 * r, 2 * p + odd] = result[:rows]
            ob[2 * r + 1, 2 * p + odd] = result[rows:]
            if split or odd:
                for h in (2 * p + odd,) if split else (2 * p, 2 * p + 1):
                    send(*output_send(2 * r, h))
                    send(*output_send(2 * r + 1, h))
        return carry

    lax.fori_loop(0, 4 * pairs - 1, query_step, 0)
    query_step(jnp.int32(4 * pairs - 1), 0, True)

    for args in own_sends:
        sent(*args)

    def all_sent(buf, sem, same):
        @pl.when(jnp.logical_not(same))
        def _():
            arrived(buf, sem)

        @pl.when(same)
        def _():
            arrived(buf.at[pl.ds(0, 7)], sem)

    all_sent(qb, q_send, home == m)

    arrived(latb.at[pl.ds(0, 31)], lat_send)
    arrived(rkb.at[pl.ds(0, 31)], rk_send)

    square = jnp.zeros((rows, 1), jnp.float32)
    for h in range(4):
        for t in range(8):
            arrived(orecv.at[t, h], o_recv.at[t, h])
            gated = orecv[t, h].astype(jnp.float32) * silu_v[t * 4 + h]
            silu_v[t * 4 + h] = gated
            square = square + jnp.sum(gated * gated, axis=-1, keepdims=True)
    scale = lax.rsqrt(square / (HEADS * VDIM) + EPS)
    outs = []
    for i in range(HEADS):
        cols = slice(i * VDIM, (i + 1) * VDIM)
        gate_v[:, cols] = (silu_v[i] * scale * ogain_ref[:, cols]).astype(jnp.bfloat16)
        if i % 8 == 7:
            cols = pl.ds(i // 8 * 1024, 1024)
            outs.append(
                pltpu.make_async_copy(gate_v.at[:, cols], out_ref.at[:, cols], out_sem.at[i // 8])
            )
            outs[-1].start()

    all_sent(ob, o_send, seq == d)
    for copy in outs:
        copy.wait()


def angle_tables(rows, n_s):
    half = ROPE // 2
    base = THETA ** (-np.arange(half) / half)
    inverse = np.zeros(128)
    inverse[:ROPE] = np.tile(base, 2)

    def both(angles):
        return np.stack([np.cos(angles), np.sin(angles)]).astype(np.float32)

    inner, outer = np.arange(rows), np.arange(n_s) * rows
    return (
        both(inner[:, None] * inverse[None, :]),
        both(outer[:, None] * inverse[None, :])[:, :, None, :],
        both(base[:, None] * inner[None, :]),
    )


def per_device(n_s, n_d, queries, latent, rope_key, latent_gain, kv_weight, gate, out_gain):
    rows, rank = latent.shape
    heads = HEADS // n_d
    pairs = heads // 2
    seq = rows * n_s
    tables = [jnp.asarray(t) for t in angle_tables(rows, n_s)]
    bf = jnp.bfloat16
    dma = pltpu.SemaphoreType.DMA
    vmem = pl.BlockSpec(memory_space=pltpu.VMEM)
    hbm = pl.BlockSpec(memory_space=pl.ANY)
    return pl.pallas_call(
        kernel,
        out_shape=jax.ShapeDtypeStruct(gate.shape, bf),
        in_specs=[hbm, vmem, vmem, vmem, hbm, hbm, vmem, vmem, vmem, vmem],
        out_specs=hbm,
        scratch_shapes=[
            pltpu.VMEM(kv_weight.shape, bf),
            pltpu.VMEM(queries.shape, bf),
            pltpu.VMEM(gate.shape, bf),
            pltpu.VMEM((HEADS, rows, VDIM), jnp.float32),
            pltpu.VMEM((rows, rank), bf),
            pltpu.VMEM((ROPE, rows), bf),
            pltpu.VMEM((n_s, rows, rank), bf),
            pltpu.VMEM((n_s, ROPE, rows), bf),
            pltpu.VMEM((n_d, pairs, rows, PAIR), bf),
            pltpu.VMEM((heads, seq, KDIM), bf),
            pltpu.VMEM((heads, seq, 2 * VDIM), bf),
            pltpu.VMEM((n_d, heads, rows, VDIM), bf),
            pltpu.VMEM((n_d, heads, rows, VDIM), bf),
            dma, dma, dma, dma((4,)), dma((len(PIECES) + 1,)),
            dma, dma((16, len(PIECES))), dma((16,)), dma, dma((16, 2)),
            dma, dma((n_d, pairs)), dma, dma((n_d, heads)),
        ],
        compiler_params=pltpu.CompilerParams(
            has_side_effects=True, collective_id=0, vmem_limit_bytes=60 * 1024 * 1024
        ),
        name="latent_attention",
    )(
        queries, latent, rope_key.T, latent_gain[None, :], kv_weight, gate, out_gain[None, :],
        *tables,
    )


def solution(mesh):
    return jax.shard_map(
        functools.partial(per_device, mesh.shape["sp"], mesh.shape["dp"]),
        mesh=mesh,
        in_specs=(
            P(("dp", "sp"), None),
            P(("dp", "sp"), None),
            P(("dp", "sp"), None),
            P(),
            P(None, "dp"),
            P(("dp", "sp"), None),
            P(),
        ),
        out_specs=P(("dp", "sp"), None),
        check_vma=False,
    )
```
